32 devices in a mesh: kv: 8 (over z, y), tp: 4 (over x, core).
Axes of the slice: x: 2, y: 2, z: 4, core: 2. Of those that a mesh axis runs over, the one named last changes fastest.
Arguments:
- layer_input: bfloat16 [4, 4096, 2048], P(None, 'kv', 'tp'), may hold values from -0.119628906 to 0.119628906
- queries: bfloat16 [4, 4096, 2048], P(None, 'kv', 'tp'), may hold values from -3.5 to 3.5
- keys: bfloat16 [4, 4096, 2048], P(None, 'kv', 'tp'), may hold values from -3.5 to 3.5
- values: bfloat16 [4, 4096, 2048], P(None, 'kv', 'tp'), may hold values from -5 to 5
- outputs: bfloat16 [4, 4096, 2048], P(None, 'kv', 'tp'), may hold values from -1.5 to 1.5
- d_out: bfloat16 [4, 4096, 2048], P(None, 'kv', 'tp'), may hold values from -30 to 30
- log_sums: float32 [4, 4096, 16], P(None, 'kv', 'tp'), may hold values from 6 to 8
- chosen: int32 [4, 64, 12], P(None, 'kv'), may hold values from -1 to 63, as said below
Outputs:
- d_queries: bfloat16 [4, 4096, 2048], P(None, 'kv', 'tp')
- d_keys: bfloat16 [4, 4096, 2048], P(None, 'kv', 'tp')
- d_values: bfloat16 [4, 4096, 2048], P(None, 'kv', 'tp')
- d_weight: float32 [2048, 2048], P('kv', 'tp')
The draws below stay inside these ranges and needn't reach their ends.
Inputs may be any that keep to these rules, and one draw needn't show every extreme that they name: Row chosen[s, b] names key blocks of sequence s for query block b: its first entry is b itself, the others are distinct blocks with smaller indices, either on the same device as b or on earlier devices; -1 marks unused slots, which come last. Over all sequences, the blocks of one device that query blocks of other devices name are at most 2, and in every draw some devices' are exactly 2.
All inputs are finite; a program needn't handle non-finite values.
Results may differ from the reference program's by a relative error of at most 0.0055.
Values may be sent and summed in bfloat16 or wider, within the bound.
A program may use at most 256 MiB of HBM per device.

```python
import jax
import jax.numpy as jnp
from jax import lax

D = 2048
HEADS = 16
DH = 128
HD = 2048
BLK = 64
SEL = 12
CAP = 2
SEQS = 4
TOK_DEV = 512
NPOS = 4096
NBLK = 64


def draw_chosen(key, part):
    local_blocks = TOK_DEV // BLK
    devices = NBLK // local_blocks
    own_blocks = SEQS * local_blocks
    pool_size = local_blocks + devices * CAP
    publish_key = jax.random.fold_in(key, 11)
    choose_key = jax.random.fold_in(key, 12)
    ranking = jax.random.randint(publish_key, (devices, own_blocks), 0, 4096) * own_blocks
    ranking = ranking + jnp.arange(own_blocks, dtype=jnp.int32)[None, :]
    published = jnp.argsort(-ranking, axis=1)[:, :CAP].astype(jnp.int32)
    owner_ids = jnp.arange(devices, dtype=jnp.int32)
    remote_seq = (published // local_blocks).reshape(devices * CAP)
    remote_block = (owner_ids[:, None] * local_blocks + published % local_blocks).reshape(devices * CAP)
    remote_owner = jnp.repeat(owner_ids, CAP)
    sequence_ids = jnp.arange(SEQS, dtype=jnp.int32)[:, None, None]
    query_block = jnp.arange(NBLK, dtype=jnp.int32)[None, :, None]
    query_device = query_block // local_blocks
    query_local = query_block % local_blocks
    local_index = jnp.arange(local_blocks, dtype=jnp.int32)[None, None, :]
    local_extent = (SEQS, NBLK, local_blocks)
    remote_extent = (SEQS, NBLK, devices * CAP)
    local_block = jnp.broadcast_to(query_device * local_blocks + local_index, local_extent)
    local_ok = jnp.broadcast_to(local_index <= query_local, local_extent)
    local_level = jnp.broadcast_to((local_index == query_local).astype(jnp.int32) * 4, local_extent)
    remote_ok = (remote_owner[None, None, :] < query_device) & (remote_seq[None, None, :] == sequence_ids)
    nearby = (remote_owner[None, None, :] == query_device - 1) | (remote_owner[None, None, :] == query_device - devices // 2)
    remote_level = jnp.broadcast_to(nearby.astype(jnp.int32) * 2, remote_extent)
    blocks = jnp.concatenate([local_block, jnp.broadcast_to(remote_block[None, None, :], remote_extent)], axis=2)
    usable = jnp.concatenate([local_ok, jnp.broadcast_to(remote_ok, remote_extent)], axis=2)
    levels = jnp.concatenate([local_level, remote_level], axis=2)
    slot_ids = jnp.arange(pool_size, dtype=jnp.int32)
    jitter = jax.random.randint(choose_key, (SEQS, NBLK, pool_size), 0, 4096)
    scores = (levels * 4096 + jitter) * pool_size + slot_ids
    scores = jnp.where(usable, scores, -1 - slot_ids)
    ranked = jnp.argsort(-scores, axis=2)[:, :, :SEL]
    top_scores = jnp.take_along_axis(scores, ranked, axis=2)
    picked = jnp.take_along_axis(blocks, ranked, axis=2)
    return jnp.where(top_scores >= 0, picked, -1).astype(jnp.int32)


def spiked(values, key, source, target, shards_of, factor):
    owner, partner = [(jnp.arange(values.shape[axis_at]) // (values.shape[axis_at] // shards_of)).reshape([-1 if axis == axis_at else 1 for axis in range(values.ndim)]) for axis_at in (source, target)]
    chosen = jax.random.permutation(key, shards_of)[partner]
    strong = (owner == chosen) | (owner == (partner + shards_of // 2) % shards_of)
    return jnp.where(strong, factor * values, values)


def block_scale(stream_key, shape, shards, smallest, largest):
    gain, own = 1.0, jax.random.fold_in(stream_key, 6)
    for position, blocks in shards:
        draws = jnp.exp(jax.random.uniform(jax.random.fold_in(own, position), (blocks,), jnp.float32, smallest / len(shards), largest / len(shards)))
        gain = gain * jnp.repeat(draws, shape[position] // blocks).reshape([-1 if axis == position else 1 for axis in range(len(shape))])
    return gain


def normal_values(own_key, shape, scale, reach, shards=(), kind=jnp.bfloat16):
    array = scale * jax.random.normal(own_key, shape, jnp.float32)
    if shards:
        array = array * block_scale(own_key, shape, shards, -0.22, 0.18)
    return jnp.clip(array, -reach, reach).astype(kind)


def bell_draw_with(stream_key, shape, width, reach, cuts, heavy, kind=jnp.bfloat16):
    result = width * jax.random.normal(stream_key, shape, jnp.float32)
    if cuts:
        result = result * block_scale(stream_key, shape, cuts, -0.22, 0.18)
    return jnp.clip(spiked(result, jax.random.fold_in(stream_key, 3), *heavy), -reach, reach).astype(kind)


def setup_inputs(seed: int = 0) -> dict:
    seeds = jax.random.split(jax.random.key(seed), 9)
    layer_input = bell_draw_with(seeds[0], (SEQS, NPOS, D), 0.02, 0.119628906, ((1, 8), (2, 4)), (1, 2, 8, 2.0))
    queries = normal_values(seeds[1], (SEQS, NPOS, HD), 0.7, 3.5, ((1, 8), (2, 4)))
    keys = normal_values(seeds[2], (SEQS, NPOS, HD), 0.7, 3.5, ((1, 8), (2, 4)))
    values = normal_values(seeds[3], (SEQS, NPOS, HD), 1.0, 5.0, ((1, 8), (2, 4)))
    outputs = normal_values(seeds[4], (SEQS, NPOS, HD), 0.25, 1.5, ((1, 8), (2, 4)))
    d_out = normal_values(seeds[5], (SEQS, NPOS, HD), 6.0, 30.0, ((1, 8), (2, 4)))
    log_sums = jnp.clip(6.0 + 2.0 * jax.random.uniform(seeds[6], (SEQS, NPOS, HEADS), jnp.float32) ** block_scale(seeds[6], (SEQS, NPOS, HEADS), ((1, 8), (2, 4)), -0.2, 0.2), 6.0, 8.0)
    chosen = draw_chosen(jax.random.fold_in(seeds[8], 71), 0)
    return dict(layer_input=layer_input, queries=queries, keys=keys, values=values, outputs=outputs, d_out=d_out, log_sums=log_sums, chosen=chosen)


def one_sequence(bundle):
    queries, keys, values, outputs, d_out, log_sums, chosen = bundle
    inverse_root = DH ** -0.5
    query_blocks = queries.reshape(NBLK, BLK, HEADS, DH)
    key_blocks = keys.reshape(NBLK, BLK, HEADS, DH)
    value_blocks = values.reshape(NBLK, BLK, HEADS, DH)
    cotangent = d_out.reshape(NBLK, BLK, HEADS, DH)
    product = d_out.astype(jnp.float32) * outputs.astype(jnp.float32)
    deltas = jnp.sum(product.reshape(NBLK, BLK, HEADS, DH), axis=3)
    log_blocks = log_sums.reshape(NBLK, BLK, HEADS)
    offsets = jnp.arange(BLK, dtype=jnp.int32)

    def advance(totals, block_index):
        key_total, value_total = totals
        picked = chosen[block_index]
        in_use = picked >= 0
        clamped = jnp.maximum(picked, 0).astype(jnp.int32)
        key_picked = key_blocks[clamped].astype(jnp.float32)
        value_picked = value_blocks[clamped].astype(jnp.float32)
        key_place = clamped[:, None] * BLK + offsets[None, :]
        query_place = block_index * BLK + offsets
        visible = in_use[None, :, None] & (key_place[None, :, :] <= query_place[:, None, None])
        query_rows = query_blocks[block_index].astype(jnp.float32)
        grad_rows = cotangent[block_index].astype(jnp.float32)
        scores = jnp.einsum('qhd,ekhd->hqek', query_rows, key_picked) * inverse_root
        log_shift = log_blocks[block_index].T[:, :, None, None]
        prob_full = jnp.where(visible[None], jnp.exp(scores - log_shift), 0.0)
        prob_grad = jnp.einsum('qhd,ekhd->hqek', grad_rows, value_picked)
        score_grad = prob_full * (prob_grad - deltas[block_index].T[:, :, None, None])
        prob_low = lax.optimization_barrier(prob_full.astype(jnp.bfloat16)).astype(jnp.float32)
        score_low = lax.optimization_barrier(score_grad.astype(jnp.bfloat16)).astype(jnp.float32)
        grad_query = jnp.einsum('hqek,ekhd->qhd', score_low, key_picked) * inverse_root
        grad_key = jnp.einsum('hqek,qhd->ekhd', score_low, query_rows) * inverse_root
        grad_value = jnp.einsum('hqek,qhd->ekhd', prob_low, grad_rows)
        weight = in_use.astype(jnp.float32)[:, None, None, None]
        key_total = key_total.at[clamped].add(grad_key * weight)
        value_total = value_total.at[clamped].add(grad_value * weight)
        return (key_total, value_total), grad_query.astype(jnp.bfloat16)

    zeroed = jnp.zeros((NBLK, BLK, HEADS, DH), jnp.float32)
    totals, grad_query = lax.scan(advance, (zeroed, zeroed), jnp.arange(NBLK, dtype=jnp.int32))
    key_total, value_total = totals
    d_queries = grad_query.reshape(NPOS, HEADS * DH)
    d_keys = key_total.astype(jnp.bfloat16).reshape(NPOS, HEADS * DH)
    d_values = value_total.astype(jnp.bfloat16).reshape(NPOS, HEADS * DH)
    return d_queries, d_keys, d_values


def reference(layer_input, queries, keys, values, outputs, d_out, log_sums, chosen):
    d_queries, d_keys, d_values = lax.map(one_sequence, (queries, keys, values, outputs, d_out, log_sums, chosen))
    flat_input = layer_input.reshape(SEQS * NPOS, D)
    flat_values = d_values.reshape(SEQS * NPOS, HEADS * DH)
    d_weight = jnp.dot(flat_input.T, flat_values, preferred_element_type=jnp.float32)
    return d_queries, d_keys, d_values, d_weight
```

```python
import functools

import jax
import jax.numpy as jnp
from jax import lax
from jax.experimental import pallas as pl
from jax.experimental.pallas import tpu as pltpu
from jax.sharding import PartitionSpec as P

BLK = 64
SEL = 12
CAP = 2
LOG2E = 1.4426950408889634
HIDDEN = 1e30
GROUP = 4

NT = (((1,), (1,)), ((), ()))
NN = (((1,), (0,)), ((), ()))
TN = (((0,), (0,)), ((), ()))


def dot(a, b, dims):
    return lax.dot_general(a, b, dims, preferred_element_type=jnp.float32)


def pair_terms(k, v, q, g, shift_rows, delta_row, scale, diagonal):
    count = q.shape[0]
    shift = jnp.concatenate([jnp.broadcast_to(r, (BLK, count)) for r in shift_rows], axis=0)
    prob = jnp.exp2(dot(k, q, NT) * (scale * LOG2E) - shift)
    if diagonal:
        rows = lax.broadcasted_iota(jnp.int32, prob.shape, 0)
        cols = lax.broadcasted_iota(jnp.int32, prob.shape, 1)
        prob = jnp.where(rows <= cols, prob, 0.0)
    dscore = prob * (dot(v, g, NT) - delta_row)
    prob = prob.astype(jnp.bfloat16)
    dscore = dscore.astype(jnp.bfloat16)
    return dot(dscore, k, TN), dot(dscore, q, NN) * scale, dot(prob, g, NN)


def local_kernel(scale, q_ref, k_ref, v_ref, o_ref, g_ref, log_ref, hide_ref,
                 dq_ref, dk_ref, dv_ref, delta_ref):
    positions = q_ref.shape[1]
    product = g_ref[0].astype(jnp.float32) * o_ref[0].astype(jnp.float32)
    delta = jnp.sum(product.T, axis=0, keepdims=True)
    delta_ref[0, 0] = delta
    log_row = log_ref[0, 0]
    chunk = GROUP * BLK
    for start in range(0, positions, chunk):
        keys = slice(start, start + chunk)
        rest = slice(start, positions)
        shifts = [
            log_row[:, rest] + hide_ref[0, start // BLK + i : start // BLK + i + 1, rest]
            for i in range(GROUP)
        ]
        dq, dk, dv = pair_terms(
            k_ref[0, keys], v_ref[0, keys], q_ref[0, rest], g_ref[0, rest],
            shifts, delta[:, rest], scale, True,
        )
        if start == 0:
            dq_ref[0] = dq
        else:
            dq_ref[0, rest] += dq
        dk_ref[0, keys] = dk.astype(jnp.bfloat16)
        dv_ref[0, keys] = dv.astype(jnp.bfloat16)


def remote_kernel(scale, order_ref, chunks_ref, pool_ref, hide_ref, q_ref, g_ref, log_ref,
                  delta_ref, base_ref, dq_ref, out_ref, total):
    s = pl.program_id(1)

    @pl.when(s == 0)
    def _():
        out_ref[...] = jnp.zeros_like(out_ref)

    total[...] = base_ref[0]

    @pl.loop(0, chunks_ref[s])
    def _(c):
        slots = [order_ref[s, c * GROUP + i] for i in range(GROUP)]
        places = [(lax.div(r, CAP), lax.rem(r, CAP)) for r in slots]
        k = jnp.concatenate([pool_ref[o, 0, n] for o, n in places], axis=0)
        v = jnp.concatenate([pool_ref[o, 1, n] for o, n in places], axis=0)
        shifts = [log_ref[0, 0] + hide_ref[r] for r in slots]
        dq, dk, dv = pair_terms(
            k, v, q_ref[0], g_ref[0], shifts, delta_ref[0, 0], scale, False
        )
        total[...] += dq
        dk = dk.astype(jnp.bfloat16)
        dv = dv.astype(jnp.bfloat16)
        for i, (o, n) in enumerate(places):
            out_ref[o, 0, n] = dk[i * BLK : (i + 1) * BLK]
            out_ref[o, 1, n] = dv[i * BLK : (i + 1) * BLK]

    dq_ref[0] = (total[...] * scale).astype(jnp.bfloat16)


def body(layer_input, queries, keys, values, outputs, d_out, log_sums, chosen):
    sequences, positions, channels = queries.shape
    head_count = log_sums.shape[2]
    head_size = channels // head_count
    local_blocks = positions // BLK
    devices = lax.axis_size("kv")
    me = lax.axis_index("kv")
    own_blocks = sequences * local_blocks
    slots = devices * CAP
    scale = head_size ** (-0.5)
    bf16, f32, i32 = jnp.bfloat16, jnp.float32, jnp.int32

    every = lax.all_gather(chosen, "kv", axis=1, tiled=True)
    whole_input = lax.all_gather(layer_input, "tp", axis=0)

    total_blocks = devices * local_blocks
    ids = jnp.arange(total_blocks, dtype=i32)
    asker = ids // local_blocks
    named = (every[..., None] == ids) & (
        asker[None, :, None, None] != asker[None, None, None, :]
    )
    needed = jnp.any(named, axis=(1, 2))
    needed = needed.reshape(sequences, devices, local_blocks).transpose(1, 0, 2)
    needed = needed.reshape(devices, own_blocks)
    place = jnp.where(needed, jnp.arange(own_blocks, dtype=i32), own_blocks)
    table = []
    for _ in range(CAP):
        first = jnp.min(place, axis=1)
        table.append(first)
        place = jnp.where(place == first[:, None], own_blocks, place)
    table = jnp.stack(table, axis=1)
    served = lax.dynamic_slice_in_dim(table, me, 1, 0).reshape(CAP)
    served = jnp.where(served < own_blocks, served, 0)

    key_rows = keys.reshape(own_blocks, BLK, channels)
    value_rows = values.reshape(own_blocks, BLK, channels)
    sent = jnp.stack([
        jnp.stack([lax.dynamic_index_in_dim(rows, served[n], 0, False) for n in range(CAP)])
        for rows in (key_rows, value_rows)
    ])
    pool = lax.all_gather(sent, "kv", axis=0)

    slot_place = table.reshape(slots)
    slot_owner = jnp.arange(slots, dtype=i32) // CAP
    slot_ok = (slot_place < own_blocks) & (slot_owner != me)
    slot_seq = jnp.where(slot_ok, slot_place // local_blocks, -1)
    slot_block = slot_owner * local_blocks + slot_place % local_blocks
    seqs = jnp.arange(sequences, dtype=i32)
    sees = jnp.any(chosen[..., None] == slot_block, axis=2) & (
        slot_seq[None, None, :] == seqs[:, None, None]
    )
    seen = jnp.any(sees, axis=0)
    remote_hide = jnp.where(seen.T, 0.0, HIDDEN).astype(f32)
    remote_hide = jnp.repeat(remote_hide, BLK, axis=1).reshape(slots, 1, positions)
    match = jnp.any(sees, axis=1)
    line = jnp.arange(slots, dtype=i32)
    rank = jnp.sum((match[:, None, :] & (line[None, None, :] < line[None, :, None])).astype(i32), axis=2)
    count = jnp.sum(match.astype(i32), axis=1)
    chunks = (count + GROUP - 1) // GROUP
    padded = -(-slots // GROUP) * GROUP
    steps = jnp.arange(padded, dtype=i32)
    hits = match[:, None, :] & (rank[:, None, :] == steps[None, :, None])
    order = jnp.sum(jnp.where(hits, line[None, None, :], 0), axis=2)
    order = jnp.where(steps[None, :] < count[:, None], order, me * CAP)

    mine = me * local_blocks + jnp.arange(local_blocks, dtype=i32)
    near = jnp.any(chosen[..., None] == mine, axis=2)
    local_hide = jnp.where(near.transpose(0, 2, 1), 0.0, HIDDEN).astype(f32)
    local_hide = jnp.repeat(local_hide, BLK, axis=2)
    log_rows = (log_sums * LOG2E).transpose(0, 2, 1)[:, :, None, :]

    tile = pl.BlockSpec((1, positions, head_size), lambda s, h: (s, 0, h))
    row = pl.BlockSpec((1, 1, 1, positions), lambda s, h: (s, h, 0, 0))
    shape = (sequences, positions, channels)
    flops = 10 * sequences * head_count * positions * positions * head_size
    dq_local, dk_local, dv_local, delta_rows = pl.pallas_call(
        functools.partial(local_kernel, scale),
        grid=(sequences, head_count),
        in_specs=[tile] * 5 + [row, pl.BlockSpec((1, local_blocks, positions), lambda s, h: (s, 0, 0))],
        out_specs=[tile, tile, tile, row],
        out_shape=[
            jax.ShapeDtypeStruct(shape, f32),
            jax.ShapeDtypeStruct(shape, bf16),
            jax.ShapeDtypeStruct(shape, bf16),
            jax.ShapeDtypeStruct((sequences, head_count, 1, positions), f32),
        ],
        cost_estimate=pl.CostEstimate(flops=4 * flops, bytes_accessed=queries.size * 18, transcendentals=0),
        name="near_terms",
    )(queries, keys, values, outputs, d_out, log_rows, local_hide)

    tile_t = pl.BlockSpec((1, positions, head_size), lambda h, s, *_: (s, 0, h))
    row_t = pl.BlockSpec((1, 1, 1, positions), lambda h, s, *_: (s, h, 0, 0))
    pool_t = pl.BlockSpec((devices, 2, CAP, BLK, head_size), lambda h, s, *_: (0, 0, 0, 0, h))
    d_queries, terms = pl.pallas_call(
        functools.partial(remote_kernel, scale),
        grid_spec=pltpu.PrefetchScalarGridSpec(
            num_scalar_prefetch=2,
            grid=(head_count, sequences),
            in_specs=[
                pool_t,
                pl.BlockSpec((slots, 1, positions), lambda h, s, *_: (0, 0, 0)),
                tile_t, tile_t, row_t, row_t, tile_t,
            ],
            out_specs=[tile_t, pool_t],
            scratch_shapes=[pltpu.VMEM((positions, head_size), f32)],
        ),
        out_shape=[
            jax.ShapeDtypeStruct(shape, bf16),
            jax.ShapeDtypeStruct((devices, 2, CAP, BLK, channels), bf16),
        ],
        cost_estimate=pl.CostEstimate(flops=2 * flops, bytes_accessed=queries.size * 10, transcendentals=0),
        name="far_terms",
    )(order, chunks, pool, remote_hide, queries, d_out, log_rows, delta_rows, dq_local)

    returned = lax.all_to_all(terms, "kv", split_axis=0, concat_axis=0, tiled=True)
    returned = jnp.sum(returned.astype(f32), axis=0)

    def settle(rows, back):
        rows = rows.reshape(own_blocks, BLK, channels)
        for n in range(CAP):
            held = lax.dynamic_index_in_dim(rows, served[n], 0, False).astype(f32)
            rows = lax.dynamic_update_index_in_dim(rows, (held + back[n]).astype(bf16), served[n], 0)
        return rows.reshape(shape)

    d_keys = settle(dk_local, returned[0])
    d_values = settle(dv_local, returned[1])
    input_rows = whole_input.reshape(-1, sequences * positions, layer_input.shape[2])
    partial = jnp.einsum(
        "pti,tj->pij", input_rows, d_values.reshape(sequences * positions, channels),
        preferred_element_type=f32,
    ).reshape(-1, channels)
    d_weight = lax.psum_scatter(partial, "kv", scatter_dimension=0, tiled=True)
    return (d_queries, d_keys, d_values, d_weight)


def solution(mesh):
    split = P(None, "kv", "tp")
    return jax.shard_map(
        body,
        mesh=mesh,
        in_specs=(split,) * 7 + (P(None, "kv", None),),
        out_specs=(split, split, split, P("kv", "tp")),
        check_vma=False,
    )
```

```python
import functools

import jax
import jax.numpy as jnp
from jax import lax
from jax.experimental import pallas as pl
from jax.experimental.pallas import tpu as pltpu
from jax.sharding import PartitionSpec as P

BLK = 64
SEL = 12
CAP = 2
LOG2E = 1.4426950408889634
HIDDEN = 1e30
GROUP = 4

NT = (((1,), (1,)), ((), ()))
NN = (((1,), (0,)), ((), ()))
TN = (((0,), (0,)), ((), ()))


def dot(a, b, dims):
    return lax.dot_general(a, b, dims, preferred_element_type=jnp.float32)


def pair_terms(k, v, q, g, shift_rows, delta_row, scale, diagonal):
    count = q.shape[0]
    shift = jnp.concatenate([jnp.broadcast_to(r, (BLK, count)) for r in shift_rows], axis=0)
    prob = jnp.exp2(dot(k, q, NT) * (scale * LOG2E) - shift)
    if diagonal:
        rows = lax.broadcasted_iota(jnp.int32, prob.shape, 0)
        cols = lax.broadcasted_iota(jnp.int32, prob.shape, 1)
        prob = jnp.where(rows <= cols, prob, 0.0)
    dscore = prob * (dot(v, g, NT) - delta_row)
    prob = prob.astype(jnp.bfloat16)
    dscore = dscore.astype(jnp.bfloat16)
    return dot(dscore, k, TN), dot(dscore, q, NN) * scale, dot(prob, g, NN)


def peer(index):
    return dict(device_id={"kv": index}, device_id_type=pl.DeviceIdType.MESH)


def meet(others):
    barrier = pltpu.get_barrier_semaphore()
    for other in others:
        pl.semaphore_signal(barrier, inc=1, **peer(other))
    pl.semaphore_wait(barrier, len(others))


def places_of(devices):
    me = lax.axis_index("kv")
    inner = 2 if devices % 2 == 0 else 1
    outer = devices // inner
    a, b = me // inner, me % inner
    onward = [lax.rem(a + 1 + i, outer) for i in range(outer)]
    source = [lax.rem(a + outer - 1 - i, outer) for i in range(outer)]
    return me, inner, outer, a, b, onward, source


def spread_kernel(devices, mine_ref, all_ref, send_sem, recv_sem):
    me = lax.axis_index("kv")
    others = [lax.rem(me + i, devices) for i in range(1, devices)]
    meet(others)
    copies = []
    for i, other in enumerate(others):
        copy = pltpu.make_async_remote_copy(
            mine_ref, all_ref.at[me], send_sem.at[i], recv_sem.at[i], **peer(other)
        )
        copy.start()
        copies.append(copy)
    all_ref[pl.ds(me, 1)] = mine_ref[...][None]
    for copy in copies:
        copy.wait()


def spread(chosen, devices):
    return pl.pallas_call(
        functools.partial(spread_kernel, devices),
        out_shape=jax.ShapeDtypeStruct((devices,) + chosen.shape, chosen.dtype),
        in_specs=[pl.BlockSpec(memory_space=pltpu.VMEM)],
        out_specs=pl.BlockSpec(memory_space=pltpu.VMEM),
        scratch_shapes=[pltpu.SemaphoreType.DMA((devices - 1,)), pltpu.SemaphoreType.DMA((devices - 1,))],
        compiler_params=pltpu.CompilerParams(collective_id=0, has_side_effects=True),
        name="spread_choice",
    )(chosen)


def total_kernel(devices, terms_ref, out_ref, near_in, far_out, far_in,
                 near_send, near_recv, far_send, far_recv):
    me, inner, outer, a, b, onward, _ = places_of(devices)
    partner = a * inner + (1 - b)
    meet([partner] + [place * inner + b for place in onward[:-1]])
    near, far = [], []
    for i, place in enumerate(onward):
        copy = pltpu.make_async_remote_copy(
            terms_ref.at[place * inner + (1 - b)], near_in.at[i],
            near_send.at[i], near_recv.at[i], **peer(partner),
        )
        copy.start()
        near.append(copy)
    for i, place in enumerate(onward):
        near[i].wait_recv()
        both = terms_ref[place * inner + b].astype(jnp.float32) + near_in[i].astype(jnp.float32)
        if i == outer - 1:
            out_ref[...] = both
            break
        far_out[i] = both.astype(jnp.bfloat16)
        copy = pltpu.make_async_remote_copy(
            far_out.at[i], far_in.at[i], far_send.at[i], far_recv.at[i],
            **peer(place * inner + b),
        )
        copy.start()
        far.append(copy)
    for i, copy in enumerate(far):
        copy.wait_recv()
        out_ref[...] += far_in[i].astype(jnp.float32)
    for copy in near + far:
        copy.wait_send()


def total(terms, ident, label):
    devices, rows, columns = terms.shape
    outer = devices // 2
    dma = pltpu.SemaphoreType.DMA
    return pl.pallas_call(
        functools.partial(total_kernel, devices),
        out_shape=jax.ShapeDtypeStruct((rows, columns), jnp.float32),
        in_specs=[pl.BlockSpec(memory_space=pltpu.VMEM)],
        out_specs=pl.BlockSpec(memory_space=pltpu.VMEM),
        scratch_shapes=[
            pltpu.VMEM((outer, rows, columns), jnp.bfloat16),
            pltpu.VMEM((outer - 1, rows, columns), jnp.bfloat16),
            pltpu.VMEM((outer - 1, rows, columns), jnp.bfloat16),
            dma((outer,)), dma((outer,)), dma((outer - 1,)), dma((outer - 1,)),
        ],
        compiler_params=pltpu.CompilerParams(collective_id=ident, has_side_effects=True),
        name=label,
    )(terms)


def gather_copies(devices, mine_ref, pool_ref, own_send, own_recv, far_send, far_recv, pass_send, pass_recv):
    me, inner, outer, a, b, onward, source = places_of(devices)
    partner = a * inner + (1 - b)
    own = pltpu.make_async_remote_copy(
        mine_ref, pool_ref.at[me], own_send, own_recv, **peer(partner)
    )
    far = [
        pltpu.make_async_remote_copy(
            mine_ref, pool_ref.at[me], far_send.at[i], far_recv.at[i],
            **peer(onward[i] * inner + b),
        )
        for i in range(outer - 1)
    ]
    onto = [
        pltpu.make_async_remote_copy(
            pool_ref.at[source[i] * inner + b], pool_ref.at[source[i] * inner + b],
            pass_send.at[i], pass_recv.at[i], **peer(partner),
        )
        for i in range(outer - 1)
    ]
    others = [partner] + [onward[i] * inner + b for i in range(outer - 1)]
    return own, far, onto, others


def local_kernel(devices, steps, scale, mine_ref, q_ref, k_ref, v_ref, o_ref, g_ref, log_ref, hide_ref,
                 dq_ref, dk_ref, dv_ref, delta_ref, pool_ref, *sems):
    positions = q_ref.shape[1]
    step = pl.program_id(0) * pl.num_programs(1) + pl.program_id(1)
    own, far, onto, others = gather_copies(devices, mine_ref, pool_ref, *sems)

    @pl.when(step == 0)
    def _():
        meet(others)
        for copy in far:
            copy.start()
        own.start()

    for i in range(len(far)):
        @pl.when(step == (i + 1) * steps // (len(far) + 1))
        def _(i=i):
            far[i].wait_recv()
            onto[i].start()

    product = g_ref[0].astype(jnp.float32) * o_ref[0].astype(jnp.float32)
    delta = jnp.sum(product.T, axis=0, keepdims=True)
    delta_ref[0, 0] = delta
    log_row = log_ref[0, 0]
    chunk = GROUP * BLK
    for start in range(0, positions, chunk):
        keys = slice(start, start + chunk)
        rest = slice(start, positions)
        shifts = [
            log_row[:, rest] + hide_ref[0, start // BLK + i : start // BLK + i + 1, rest]
            for i in range(GROUP)
        ]
        dq, dk, dv = pair_terms(
            k_ref[0, keys], v_ref[0, keys], q_ref[0, rest], g_ref[0, rest],
            shifts, delta[:, rest], scale, True,
        )
        if start == 0:
            dq_ref[0] = dq
        else:
            dq_ref[0, rest] += dq
        dk_ref[0, keys] = dk.astype(jnp.bfloat16)
        dv_ref[0, keys] = dv.astype(jnp.bfloat16)

    @pl.when(step == steps - 1)
    def _():
        own.wait()
        for copy in far:
            copy.wait_send()
        for copy in onto:
            copy.wait()


def remote_kernel(scale, order_ref, read_ref, chunks_ref, pool_ref, hide_ref, q_ref, g_ref, log_ref,
                  delta_ref, base_ref, dq_ref, out_ref, total):
    s = pl.program_id(1)

    @pl.when(s == 0)
    def _():
        out_ref[...] = jnp.zeros_like(out_ref)

    total[...] = base_ref[0]

    @pl.loop(0, chunks_ref[s])
    def _(c):
        slots = [order_ref[s, c * GROUP + i] for i in range(GROUP)]
        places = [(lax.div(r, CAP), lax.rem(r, CAP)) for r in slots]
        reads = [read_ref[s, c * GROUP + i] for i in range(GROUP)]
        reads = [(lax.div(r, CAP), lax.rem(r, CAP)) for r in reads]
        k = jnp.concatenate([pool_ref[o, 0, n] for o, n in reads], axis=0)
        v = jnp.concatenate([pool_ref[o, 1, n] for o, n in reads], axis=0)
        shifts = [log_ref[0, 0] + hide_ref[r] for r in slots]
        dq, dk, dv = pair_terms(
            k, v, q_ref[0], g_ref[0], shifts, delta_ref[0, 0], scale, False
        )
        total[...] += dq
        dk = dk.astype(jnp.bfloat16)
        dv = dv.astype(jnp.bfloat16)
        for i, (o, n) in enumerate(places):
            out_ref[o, 0, n] = dk[i * BLK : (i + 1) * BLK]
            out_ref[o, 1, n] = dv[i * BLK : (i + 1) * BLK]

    dq_ref[0] = (total[...] * scale).astype(jnp.bfloat16)


def body(layer_input, queries, keys, values, outputs, d_out, log_sums, chosen):
    sequences, positions, channels = queries.shape
    head_count = log_sums.shape[2]
    head_size = channels // head_count
    local_blocks = positions // BLK
    devices = lax.axis_size("kv")
    me = lax.axis_index("kv")
    own_blocks = sequences * local_blocks
    slots = devices * CAP
    scale = head_size ** (-0.5)
    bf16, f32, i32 = jnp.bfloat16, jnp.float32, jnp.int32

    every = spread(chosen, devices).transpose(1, 0, 2, 3).reshape(sequences, -1, chosen.shape[2])
    whole_input = lax.all_gather(layer_input, "tp", axis=0)

    total_blocks = devices * local_blocks
    ids = jnp.arange(total_blocks, dtype=i32)
    asker = ids // local_blocks
    named = (every[..., None] == ids) & (
        asker[None, :, None, None] != asker[None, None, None, :]
    )
    needed = jnp.any(named, axis=(1, 2))
    needed = needed.reshape(sequences, devices, local_blocks).transpose(1, 0, 2)
    needed = needed.reshape(devices, own_blocks)
    place = jnp.where(needed, jnp.arange(own_blocks, dtype=i32), own_blocks)
    table = []
    for _ in range(CAP):
        first = jnp.min(place, axis=1)
        table.append(first)
        place = jnp.where(place == first[:, None], own_blocks, place)
    table = jnp.stack(table, axis=1)
    served = lax.dynamic_slice_in_dim(table, me, 1, 0).reshape(CAP)
    served = jnp.where(served < own_blocks, served, 0)

    key_rows = keys.reshape(own_blocks, BLK, channels)
    value_rows = values.reshape(own_blocks, BLK, channels)
    sent = jnp.stack([
        jnp.stack([lax.dynamic_index_in_dim(rows, served[n], 0, False) for n in range(CAP)])
        for rows in (key_rows, value_rows)
    ])

    slot_place = table.reshape(slots)
    slot_owner = jnp.arange(slots, dtype=i32) // CAP
    slot_ok = (slot_place < own_blocks) & (slot_owner != me)
    slot_seq = jnp.where(slot_ok, slot_place // local_blocks, -1)
    slot_block = slot_owner * local_blocks + slot_place % local_blocks
    seqs = jnp.arange(sequences, dtype=i32)
    sees = jnp.any(chosen[..., None] == slot_block, axis=2) & (
        slot_seq[None, None, :] == seqs[:, None, None]
    )
    seen = jnp.any(sees, axis=0)
    remote_hide = jnp.where(seen.T, 0.0, HIDDEN).astype(f32)
    remote_hide = jnp.repeat(remote_hide, BLK, axis=1).reshape(slots, 1, positions)
    match = jnp.any(sees, axis=1)
    line = jnp.arange(slots, dtype=i32)
    rank = jnp.sum((match[:, None, :] & (line[None, None, :] < line[None, :, None])).astype(i32), axis=2)
    count = jnp.sum(match.astype(i32), axis=1)
    chunks = (count + GROUP - 1) // GROUP
    padded = -(-slots // GROUP) * GROUP
    steps = jnp.arange(padded, dtype=i32)
    hits = match[:, None, :] & (rank[:, None, :] == steps[None, :, None])
    order = jnp.sum(jnp.where(hits, line[None, None, :], 0), axis=2)
    filled = steps[None, :] < count[:, None]
    read = jnp.where(filled, order, (me ^ 1) * CAP)
    order = jnp.where(filled, order, me * CAP)

    mine = me * local_blocks + jnp.arange(local_blocks, dtype=i32)
    near = jnp.any(chosen[..., None] == mine, axis=2)
    local_hide = jnp.where(near.transpose(0, 2, 1), 0.0, HIDDEN).astype(f32)
    local_hide = jnp.repeat(local_hide, BLK, axis=2)
    log_rows = (log_sums * LOG2E).transpose(0, 2, 1)[:, :, None, :]

    tile = pl.BlockSpec((1, positions, head_size), lambda s, h: (s, 0, h))
    row = pl.BlockSpec((1, 1, 1, positions), lambda s, h: (s, h, 0, 0))
    shape = (sequences, positions, channels)
    flops = 10 * sequences * head_count * positions * positions * head_size
    dma = pltpu.SemaphoreType.DMA
    hops = devices // 2 - 1
    dq_local, dk_local, dv_local, delta_rows, pool = pl.pallas_call(
        functools.partial(local_kernel, devices, sequences * head_count, scale),
        grid=(sequences, head_count),
        in_specs=[pl.BlockSpec(memory_space=pl.ANY)] + [tile] * 5 + [row, pl.BlockSpec((1, local_blocks, positions), lambda s, h: (s, 0, 0))],
        out_specs=[tile, tile, tile, row, pl.BlockSpec(memory_space=pl.ANY)],
        out_shape=[
            jax.ShapeDtypeStruct(shape, f32),
            jax.ShapeDtypeStruct(shape, bf16),
            jax.ShapeDtypeStruct(shape, bf16),
            jax.ShapeDtypeStruct((sequences, head_count, 1, positions), f32),
            jax.ShapeDtypeStruct((devices, 2, CAP, BLK, channels), bf16),
        ],
        scratch_shapes=[dma, dma, dma((hops,)), dma((hops,)), dma((hops,)), dma((hops,))],
        compiler_params=pltpu.CompilerParams(collective_id=1, has_side_effects=True),
        cost_estimate=pl.CostEstimate(flops=4 * flops, bytes_accessed=queries.size * 18, transcendentals=0),
        name="near_terms",
    )(sent, queries, keys, values, outputs, d_out, log_rows, local_hide)

    tile_t = pl.BlockSpec((1, positions, head_size), lambda h, s, *_: (s, 0, h))
    row_t = pl.BlockSpec((1, 1, 1, positions), lambda h, s, *_: (s, h, 0, 0))
    pool_t = pl.BlockSpec((devices, 2, CAP, BLK, head_size), lambda h, s, *_: (0, 0, 0, 0, h))
    d_queries, terms = pl.pallas_call(
        functools.partial(remote_kernel, scale),
        grid_spec=pltpu.PrefetchScalarGridSpec(
            num_scalar_prefetch=3,
            grid=(head_count, sequences),
            in_specs=[
                pool_t,
                pl.BlockSpec((slots, 1, positions), lambda h, s, *_: (0, 0, 0)),
                tile_t, tile_t, row_t, row_t, tile_t,
            ],
            out_specs=[tile_t, pool_t],
            scratch_shapes=[pltpu.VMEM((positions, head_size), f32)],
        ),
        out_shape=[
            jax.ShapeDtypeStruct(shape, bf16),
            jax.ShapeDtypeStruct((devices, 2, CAP, BLK, channels), bf16),
        ],
        cost_estimate=pl.CostEstimate(flops=2 * flops, bytes_accessed=queries.size * 10, transcendentals=0),
        name="far_terms",
    )(order, read, chunks, pool, remote_hide, queries, d_out, log_rows, delta_rows, dq_local)

    returned = total(terms.reshape(devices, 2 * CAP * BLK, channels), 2, "return_terms")
    returned = returned.reshape(2, CAP, BLK, channels)

    def settle(rows, back):
        rows = rows.reshape(own_blocks, BLK, channels)
        for n in range(CAP):
            held = lax.dynamic_index_in_dim(rows, served[n], 0, False).astype(f32)
            rows = lax.dynamic_update_index_in_dim(rows, (held + back[n]).astype(bf16), served[n], 0)
        return rows.reshape(shape)

    d_keys = settle(dk_local, returned[0])
    d_values = settle(dv_local, returned[1])
    input_rows = whole_input.reshape(-1, sequences * positions, layer_input.shape[2])
    partial = jnp.einsum(
        "pti,tj->pij", input_rows, d_values.reshape(sequences * positions, channels),
        preferred_element_type=f32,
    ).astype(bf16).reshape(devices, -1, channels)
    d_weight = total(partial, 3, "weight_terms")
    return (d_queries, d_keys, d_values, d_weight)


def solution(mesh):
    split = P(None, "kv", "tp")
    return jax.shard_map(
        body,
        mesh=mesh,
        in_specs=(split,) * 7 + (P(None, "kv", None),),
        out_specs=(split, split, split, P("kv", "tp")),
        check_vma=False,
    )
```

```python
import functools

import jax
import jax.numpy as jnp
from jax import lax
from jax.experimental import pallas as pl
from jax.experimental.pallas import tpu as pltpu
from jax.sharding import PartitionSpec as P

BLK = 64
SEL = 12
CAP = 2
LOG2E = 1.4426950408889634
HIDDEN = 1e30
GROUP = 4

NT = (((1,), (1,)), ((), ()))
NN = (((1,), (0,)), ((), ()))
TN = (((0,), (0,)), ((), ()))


def dot(a, b, dims):
    return lax.dot_general(a, b, dims, preferred_element_type=jnp.float32)


def pair_terms(k, v, q, g, shift_rows, delta_row, scale, diagonal):
    count = q.shape[0]
    shift = jnp.concatenate([jnp.broadcast_to(r, (BLK, count)) for r in shift_rows], axis=0)
    prob = jnp.exp2(dot(k, q, NT) * (scale * LOG2E) - shift)
    if diagonal:
        rows = lax.broadcasted_iota(jnp.int32, prob.shape, 0)
        cols = lax.broadcasted_iota(jnp.int32, prob.shape, 1)
        prob = jnp.where(rows <= cols, prob, 0.0)
    dscore = prob * (dot(v, g, NT) - delta_row)
    prob = prob.astype(jnp.bfloat16)
    dscore = dscore.astype(jnp.bfloat16)
    return dot(dscore, k, TN), dot(dscore, q, NN) * scale, dot(prob, g, NN)


def peer(index, axis="kv"):
    return dict(device_id={axis: index}, device_id_type=pl.DeviceIdType.MESH)


def meet(others, across=()):
    barrier = pltpu.get_barrier_semaphore()
    for other in others:
        pl.semaphore_signal(barrier, inc=1, **peer(other))
    for other in across:
        pl.semaphore_signal(barrier, inc=1, **peer(other, "tp"))
    pl.semaphore_wait(barrier, len(others) + len(across))


def places_of(devices, axis="kv"):
    me = lax.axis_index(axis)
    inner = 2 if devices % 2 == 0 else 1
    outer = devices // inner
    a, b = me // inner, me % inner
    onward = [lax.rem(a + 1 + i, outer) for i in range(outer)]
    source = [lax.rem(a + outer - 1 - i, outer) for i in range(outer)]
    return me, inner, outer, a, b, onward, source


def spread_kernel(devices, mine_ref, all_ref, send_sem, recv_sem):
    me = lax.axis_index("kv")
    others = [lax.rem(me + i, devices) for i in range(1, devices)]
    meet(others)
    copies = []
    for i, other in enumerate(others):
        copy = pltpu.make_async_remote_copy(
            mine_ref, all_ref.at[me], send_sem.at[i], recv_sem.at[i], **peer(other)
        )
        copy.start()
        copies.append(copy)
    all_ref[pl.ds(me, 1)] = mine_ref[...][None]
    for copy in copies:
        copy.wait()


def spread(chosen, devices):
    return pl.pallas_call(
        functools.partial(spread_kernel, devices),
        out_shape=jax.ShapeDtypeStruct((devices,) + chosen.shape, chosen.dtype),
        in_specs=[pl.BlockSpec(memory_space=pltpu.VMEM)],
        out_specs=pl.BlockSpec(memory_space=pltpu.VMEM),
        scratch_shapes=[pltpu.SemaphoreType.DMA((devices - 1,)), pltpu.SemaphoreType.DMA((devices - 1,))],
        compiler_params=pltpu.CompilerParams(collective_id=0, has_side_effects=True),
        name="spread_choice",
    )(chosen)


def total_kernel(devices, width, *refs):
    if width:
        terms_ref, x_ref, _, out_ref, whole_ref = refs[:5]
        scratch = refs[5:12]
        half = x_ref.shape[0] // 2
        keep, (x_own, x_far, x_onto, across) = input_copies(
            width, half, x_ref.shape[0] - half, x_ref, whole_ref, *refs[12:]
        )
    else:
        terms_ref, out_ref = refs[:2]
        scratch = refs[2:]
        across = ()
    near_in, far_out, far_in, near_send, near_recv, far_send, far_recv = scratch
    me, inner, outer, a, b, onward, _ = places_of(devices)
    partner = a * inner + (1 - b)
    meet([partner] + [place * inner + b for place in onward[:-1]], across)
    near, far = [], []
    for i, place in enumerate(onward):
        copy = pltpu.make_async_remote_copy(
            terms_ref.at[place * inner + (1 - b)], near_in.at[i],
            near_send.at[i], near_recv.at[i], **peer(partner),
        )
        copy.start()
        near.append(copy)
    if width:
        for copy in x_far + [x_own, keep]:
            copy.start()
    for i, place in enumerate(onward):
        near[i].wait_recv()
        both = terms_ref[place * inner + b].astype(jnp.float32) + near_in[i].astype(jnp.float32)
        if i == outer - 1:
            out_ref[...] = both
            break
        far_out[i] = both.astype(jnp.bfloat16)
        copy = pltpu.make_async_remote_copy(
            far_out.at[i], far_in.at[i], far_send.at[i], far_recv.at[i],
            **peer(place * inner + b),
        )
        copy.start()
        far.append(copy)
    if width:
        for i in range(len(x_far)):
            x_far[i].wait_recv()
            x_onto[i].start()
    for i, copy in enumerate(far):
        copy.wait_recv()
        out_ref[...] += far_in[i].astype(jnp.float32)
    for copy in near + far:
        copy.wait_send()
    if width:
        keep.wait()
        x_own.wait()
        for copy in x_far:
            copy.wait_send()
        for copy in x_onto:
            copy.wait()


def total(terms, ident, label, layer_input=None, whole=None):
    devices, rows, columns = terms.shape
    outer = devices // 2
    dma = pltpu.SemaphoreType.DMA
    vmem, anywhere = pl.BlockSpec(memory_space=pltpu.VMEM), pl.BlockSpec(memory_space=pl.ANY)
    out_shape = [jax.ShapeDtypeStruct((rows, columns), jnp.float32)]
    scratch = [
        pltpu.VMEM((outer, rows, columns), jnp.bfloat16),
        pltpu.VMEM((outer - 1, rows, columns), jnp.bfloat16),
        pltpu.VMEM((outer - 1, rows, columns), jnp.bfloat16),
        dma((outer,)), dma((outer,)), dma((outer - 1,)), dma((outer - 1,)),
    ]
    width, more, aliases = 0, [], {}
    if whole is not None:
        width = whole.shape[0]
        more, aliases = [layer_input, whole], {2: 1}
        out_shape.append(jax.ShapeDtypeStruct(whole.shape, whole.dtype))
        scratch += [dma] + gather_sems(width)
    return pl.pallas_call(
        functools.partial(total_kernel, devices, width),
        out_shape=out_shape,
        in_specs=[vmem] + [anywhere] * len(more),
        out_specs=[vmem] + [anywhere] * (len(out_shape) - 1),
        scratch_shapes=scratch,
        input_output_aliases=aliases,
        compiler_params=pltpu.CompilerParams(collective_id=ident, has_side_effects=True),
        name=label,
    )(terms, *more)


def gather_copies(devices, axis, mine, pool, own_send, own_recv, far_send, far_recv, pass_send, pass_recv):
    me, inner, outer, a, b, onward, source = places_of(devices, axis)
    partner = a * inner + (1 - b)
    own = pltpu.make_async_remote_copy(mine, pool(me), own_send, own_recv, **peer(partner, axis))
    far = [
        pltpu.make_async_remote_copy(
            mine, pool(me), far_send.at[i], far_recv.at[i], **peer(onward[i] * inner + b, axis)
        )
        for i in range(outer - 1)
    ]
    onto = [
        pltpu.make_async_remote_copy(
            pool(source[i] * inner + b), pool(source[i] * inner + b),
            pass_send.at[i], pass_recv.at[i], **peer(partner, axis),
        )
        for i in range(outer - 1)
    ]
    others = [partner] + [onward[i] * inner + b for i in range(outer - 1)]
    return own, far, onto, others


def gather_sems(devices):
    dma, hops = pltpu.SemaphoreType.DMA, devices // 2 - 1
    return [dma, dma, dma((hops,)), dma((hops,)), dma((hops,)), dma((hops,))]


def input_copies(width, start, count, x_ref, whole_ref, keep_sem, *sems):
    part = pl.ds(start, count)
    keep = pltpu.make_async_copy(x_ref.at[part], whole_ref.at[lax.axis_index("tp"), part], keep_sem)
    return keep, gather_copies(
        width, "tp", x_ref.at[part], lambda place: whole_ref.at[place, part], *sems
    )


def local_kernel(devices, width, steps, scale, mine_ref, x_ref, q_ref, k_ref, v_ref, o_ref, g_ref, log_ref, hide_ref,
                 dq_ref, dk_ref, dv_ref, delta_ref, pool_ref, whole_ref, *sems):
    positions = q_ref.shape[1]
    step = pl.program_id(0) * pl.num_programs(1) + pl.program_id(1)
    own, far, onto, others = gather_copies(
        devices, "kv", mine_ref, lambda place: pool_ref.at[place], *sems[:6]
    )
    keep, (x_own, x_far, x_onto, across) = input_copies(
        width, 0, x_ref.shape[0] // 2, x_ref, whole_ref, *sems[6:]
    )

    @pl.when(step == 0)
    def _():
        meet(others, across)
        for copy in far:
            copy.start()
        own.start()
        for copy in x_far + [x_own, keep]:
            copy.start()

    for i in range(len(far)):
        @pl.when(step == (i + 1) * steps // (len(far) + 1))
        def _(i=i):
            far[i].wait_recv()
            onto[i].start()

    product = g_ref[0].astype(jnp.float32) * o_ref[0].astype(jnp.float32)
    delta = jnp.sum(product.T, axis=0, keepdims=True)
    delta_ref[0, 0] = delta
    log_row = log_ref[0, 0]
    chunk = GROUP * BLK
    for start in range(0, positions, chunk):
        keys = slice(start, start + chunk)
        rest = slice(start, positions)
        shifts = [
            log_row[:, rest] + hide_ref[0, start // BLK + i : start // BLK + i + 1, rest]
            for i in range(GROUP)
        ]
        dq, dk, dv = pair_terms(
            k_ref[0, keys], v_ref[0, keys], q_ref[0, rest], g_ref[0, rest],
            shifts, delta[:, rest], scale, True,
        )
        if start == 0:
            dq_ref[0] = dq
        else:
            dq_ref[0, rest] += dq
        dk_ref[0, keys] = dk.astype(jnp.bfloat16)
        dv_ref[0, keys] = dv.astype(jnp.bfloat16)

    @pl.when(step == steps - 1)
    def _():
        own.wait()
        for copy in far:
            copy.wait_send()
        for copy in x_far:
            copy.wait_recv()
        for copy in x_onto:
            copy.start()
        for copy in onto:
            copy.wait()
        keep.wait()
        x_own.wait()
        for copy in x_far:
            copy.wait_send()
        for copy in x_onto:
            copy.wait()


def remote_kernel(scale, order_ref, read_ref, chunks_ref, pool_ref, hide_ref, q_ref, g_ref, log_ref,
                  delta_ref, base_ref, dq_ref, out_ref, total):
    s = pl.program_id(1)

    @pl.when(s == 0)
    def _():
        out_ref[...] = jnp.zeros_like(out_ref)

    total[...] = base_ref[0]

    @pl.loop(0, chunks_ref[s])
    def _(c):
        slots = [order_ref[s, c * GROUP + i] for i in range(GROUP)]
        places = [(lax.div(r, CAP), lax.rem(r, CAP)) for r in slots]
        reads = [read_ref[s, c * GROUP + i] for i in range(GROUP)]
        reads = [(lax.div(r, CAP), lax.rem(r, CAP)) for r in reads]
        k = jnp.concatenate([pool_ref[o, 0, n] for o, n in reads], axis=0)
        v = jnp.concatenate([pool_ref[o, 1, n] for o, n in reads], axis=0)
        shifts = [log_ref[0, 0] + hide_ref[r] for r in slots]
        dq, dk, dv = pair_terms(
            k, v, q_ref[0], g_ref[0], shifts, delta_ref[0, 0], scale, False
        )
        total[...] += dq
        dk = dk.astype(jnp.bfloat16)
        dv = dv.astype(jnp.bfloat16)
        for i, (o, n) in enumerate(places):
            out_ref[o, 0, n] = dk[i * BLK : (i + 1) * BLK]
            out_ref[o, 1, n] = dv[i * BLK : (i + 1) * BLK]

    dq_ref[0] = (total[...] * scale).astype(jnp.bfloat16)


def body(layer_input, queries, keys, values, outputs, d_out, log_sums, chosen):
    sequences, positions, channels = queries.shape
    head_count = log_sums.shape[2]
    head_size = channels // head_count
    local_blocks = positions // BLK
    devices = lax.axis_size("kv")
    me = lax.axis_index("kv")
    own_blocks = sequences * local_blocks
    slots = devices * CAP
    scale = head_size ** (-0.5)
    bf16, f32, i32 = jnp.bfloat16, jnp.float32, jnp.int32

    every = spread(chosen, devices).transpose(1, 0, 2, 3).reshape(sequences, -1, chosen.shape[2])
    width = lax.axis_size("tp")

    total_blocks = devices * local_blocks
    ids = jnp.arange(total_blocks, dtype=i32)
    asker = ids // local_blocks
    named = (every[..., None] == ids) & (
        asker[None, :, None, None] != asker[None, None, None, :]
    )
    needed = jnp.any(named, axis=(1, 2))
    needed = needed.reshape(sequences, devices, local_blocks).transpose(1, 0, 2)
    needed = needed.reshape(devices, own_blocks)
    place = jnp.where(needed, jnp.arange(own_blocks, dtype=i32), own_blocks)
    table = []
    for _ in range(CAP):
        first = jnp.min(place, axis=1)
        table.append(first)
        place = jnp.where(place == first[:, None], own_blocks, place)
    table = jnp.stack(table, axis=1)
    served = lax.dynamic_slice_in_dim(table, me, 1, 0).reshape(CAP)
    served = jnp.where(served < own_blocks, served, 0)

    key_rows = keys.reshape(own_blocks, BLK, channels)
    value_rows = values.reshape(own_blocks, BLK, channels)
    sent = jnp.stack([
        jnp.stack([lax.dynamic_index_in_dim(rows, served[n], 0, False) for n in range(CAP)])
        for rows in (key_rows, value_rows)
    ])

    slot_place = table.reshape(slots)
    slot_owner = jnp.arange(slots, dtype=i32) // CAP
    slot_ok = (slot_place < own_blocks) & (slot_owner != me)
    slot_seq = jnp.where(slot_ok, slot_place // local_blocks, -1)
    slot_block = slot_owner * local_blocks + slot_place % local_blocks
    seqs = jnp.arange(sequences, dtype=i32)
    sees = jnp.any(chosen[..., None] == slot_block, axis=2) & (
        slot_seq[None, None, :] == seqs[:, None, None]
    )
    seen = jnp.any(sees, axis=0)
    remote_hide = jnp.where(seen.T, 0.0, HIDDEN).astype(f32)
    remote_hide = jnp.repeat(remote_hide, BLK, axis=1).reshape(slots, 1, positions)
    match = jnp.any(sees, axis=1)
    line = jnp.arange(slots, dtype=i32)
    rank = jnp.sum((match[:, None, :] & (line[None, None, :] < line[None, :, None])).astype(i32), axis=2)
    count = jnp.sum(match.astype(i32), axis=1)
    chunks = (count + GROUP - 1) // GROUP
    padded = -(-slots // GROUP) * GROUP
    steps = jnp.arange(padded, dtype=i32)
    hits = match[:, None, :] & (rank[:, None, :] == steps[None, :, None])
    order = jnp.sum(jnp.where(hits, line[None, None, :], 0), axis=2)
    filled = steps[None, :] < count[:, None]
    read = jnp.where(filled, order, (me ^ 1) * CAP)
    order = jnp.where(filled, order, me * CAP)

    mine = me * local_blocks + jnp.arange(local_blocks, dtype=i32)
    near = jnp.any(chosen[..., None] == mine, axis=2)
    local_hide = jnp.where(near.transpose(0, 2, 1), 0.0, HIDDEN).astype(f32)
    local_hide = jnp.repeat(local_hide, BLK, axis=2)
    log_rows = (log_sums * LOG2E).transpose(0, 2, 1)[:, :, None, :]

    tile = pl.BlockSpec((1, positions, head_size), lambda s, h: (s, 0, h))
    row = pl.BlockSpec((1, 1, 1, positions), lambda s, h: (s, h, 0, 0))
    shape = (sequences, positions, channels)
    flops = 10 * sequences * head_count * positions * positions * head_size
    anywhere = pl.BlockSpec(memory_space=pl.ANY)
    dq_local, dk_local, dv_local, delta_rows, pool, whole_input = pl.pallas_call(
        functools.partial(local_kernel, devices, width, sequences * head_count, scale),
        grid=(sequences, head_count),
        in_specs=[anywhere] * 2 + [tile] * 5 + [row, pl.BlockSpec((1, local_blocks, positions), lambda s, h: (s, 0, 0))],
        out_specs=[tile, tile, tile, row, anywhere, anywhere],
        out_shape=[
            jax.ShapeDtypeStruct(shape, f32),
            jax.ShapeDtypeStruct(shape, bf16),
            jax.ShapeDtypeStruct(shape, bf16),
            jax.ShapeDtypeStruct((sequences, head_count, 1, positions), f32),
            jax.ShapeDtypeStruct((devices, 2, CAP, BLK, channels), bf16),
            jax.ShapeDtypeStruct((width,) + layer_input.shape, bf16),
        ],
        scratch_shapes=gather_sems(devices) + [pltpu.SemaphoreType.DMA] + gather_sems(width),
        compiler_params=pltpu.CompilerParams(collective_id=1, has_side_effects=True),
        cost_estimate=pl.CostEstimate(flops=4 * flops, bytes_accessed=queries.size * 18, transcendentals=0),
        name="near_terms",
    )(sent, layer_input, queries, keys, values, outputs, d_out, log_rows, local_hide)

    tile_t = pl.BlockSpec((1, positions, head_size), lambda h, s, *_: (s, 0, h))
    row_t = pl.BlockSpec((1, 1, 1, positions), lambda h, s, *_: (s, h, 0, 0))
    pool_t = pl.BlockSpec((devices, 2, CAP, BLK, head_size), lambda h, s, *_: (0, 0, 0, 0, h))
    d_queries, terms = pl.pallas_call(
        functools.partial(remote_kernel, scale),
        grid_spec=pltpu.PrefetchScalarGridSpec(
            num_scalar_prefetch=3,
            grid=(head_count, sequences),
            in_specs=[
                pool_t,
                pl.BlockSpec((slots, 1, positions), lambda h, s, *_: (0, 0, 0)),
                tile_t, tile_t, row_t, row_t, tile_t,
            ],
            out_specs=[tile_t, pool_t],
            scratch_shapes=[pltpu.VMEM((positions, head_size), f32)],
        ),
        out_shape=[
            jax.ShapeDtypeStruct(shape, bf16),
            jax.ShapeDtypeStruct((devices, 2, CAP, BLK, channels), bf16),
        ],
        cost_estimate=pl.CostEstimate(flops=2 * flops, bytes_accessed=queries.size * 10, transcendentals=0),
        name="far_terms",
    )(order, read, chunks, pool, remote_hide, queries, d_out, log_rows, delta_rows, dq_local)

    returned, whole_input = total(
        terms.reshape(devices, 2 * CAP * BLK, channels), 2, "return_terms", layer_input, whole_input
    )
    returned = returned.reshape(2, CAP, BLK, channels)

    def settle(rows, back):
        rows = rows.reshape(own_blocks, BLK, channels)
        for n in range(CAP):
            held = lax.dynamic_index_in_dim(rows, served[n], 0, False).astype(f32)
            rows = lax.dynamic_update_index_in_dim(rows, (held + back[n]).astype(bf16), served[n], 0)
        return rows.reshape(shape)

    d_keys = settle(dk_local, returned[0])
    d_values = settle(dv_local, returned[1])
    input_rows = whole_input.reshape(-1, sequences * positions, layer_input.shape[2])
    partial = jnp.einsum(
        "pti,tj->pij", input_rows, d_values.reshape(sequences * positions, channels),
        preferred_element_type=f32,
    ).astype(bf16).reshape(devices, -1, channels)
    d_weight, = total(partial, 3, "weight_terms")
    return (d_queries, d_keys, d_values, d_weight)


def solution(mesh):
    split = P(None, "kv", "tp")
    return jax.shard_map(
        body,
        mesh=mesh,
        in_specs=(split,) * 7 + (P(None, "kv", None),),
        out_specs=(split, split, split, P("kv", "tp")),
        check_vma=False,
    )
```

```python
import functools

import jax
import jax.numpy as jnp
from jax import lax
from jax.experimental import pallas as pl
from jax.experimental.pallas import tpu as pltpu
from jax.sharding import PartitionSpec as P

BLK = 64
SEL = 12
CAP = 2
LOG2E = 1.4426950408889634
HIDDEN = 1e30
GROUP = 4

NT = (((1,), (1,)), ((), ()))
NN = (((1,), (0,)), ((), ()))
TN = (((0,), (0,)), ((), ()))


def dot(a, b, dims):
    return lax.dot_general(a, b, dims, preferred_element_type=jnp.float32)


def pair_terms(k, v, q, g, shift_rows, delta_row, scale, diagonal):
    count = q.shape[0]
    shift = jnp.concatenate([jnp.broadcast_to(r, (BLK, count)) for r in shift_rows], axis=0)
    prob = jnp.exp2(dot(k, q, NT) * (scale * LOG2E) - shift)
    if diagonal:
        rows = lax.broadcasted_iota(jnp.int32, prob.shape, 0)
        cols = lax.broadcasted_iota(jnp.int32, prob.shape, 1)
        prob = jnp.where(rows <= cols, prob, 0.0)
    dscore = prob * (dot(v, g, NT) - delta_row)
    prob = prob.astype(jnp.bfloat16)
    dscore = dscore.astype(jnp.bfloat16)
    return dot(dscore, k, TN), dot(dscore, q, NN) * scale, dot(prob, g, NN)


def peer(index, axis="kv"):
    return dict(device_id={axis: index}, device_id_type=pl.DeviceIdType.MESH)


def meet(others, across=()):
    barrier = pltpu.get_barrier_semaphore()
    for other in others:
        pl.semaphore_signal(barrier, inc=1, **peer(other))
    for other in across:
        pl.semaphore_signal(barrier, inc=1, **peer(other, "tp"))
    pl.semaphore_wait(barrier, len(others) + len(across))


def places_of(devices, axis="kv"):
    me = lax.axis_index(axis)
    inner = 2 if devices % 2 == 0 else 1
    outer = devices // inner
    a, b = me // inner, me % inner
    onward = [lax.rem(a + 1 + i, outer) for i in range(outer)]
    source = [lax.rem(a + outer - 1 - i, outer) for i in range(outer)]
    return me, inner, outer, a, b, onward, source


def spread_kernel(devices, mine_ref, all_ref, send_sem, recv_sem):
    me = lax.axis_index("kv")
    others = [lax.rem(me + i, devices) for i in range(1, devices)]
    meet(others)
    copies = []
    for i, other in enumerate(others):
        copy = pltpu.make_async_remote_copy(
            mine_ref, all_ref.at[me], send_sem.at[i], recv_sem.at[i], **peer(other)
        )
        copy.start()
        copies.append(copy)
    all_ref[pl.ds(me, 1)] = mine_ref[...][None]
    for copy in copies:
        copy.wait()


def spread(chosen, devices):
    return pl.pallas_call(
        functools.partial(spread_kernel, devices),
        out_shape=jax.ShapeDtypeStruct((devices,) + chosen.shape, chosen.dtype),
        in_specs=[pl.BlockSpec(memory_space=pltpu.VMEM)],
        out_specs=pl.BlockSpec(memory_space=pltpu.VMEM),
        scratch_shapes=[pltpu.SemaphoreType.DMA((devices - 1,)), pltpu.SemaphoreType.DMA((devices - 1,))],
        compiler_params=pltpu.CompilerParams(collective_id=0, has_side_effects=True),
        name="spread_choice",
    )(chosen)


def total_kernel(devices, width, *refs):
    if width:
        terms_ref, x_ref, _, out_ref, whole_ref = refs[:5]
        scratch = refs[5:12]
        half = x_ref.shape[0] // 2
        keep, (x_own, x_far, x_onto, across) = input_copies(
            width, half, x_ref.shape[0] - half, x_ref, whole_ref, *refs[12:]
        )
    else:
        terms_ref, out_ref = refs[:2]
        scratch = refs[2:]
        across = ()
    near_in, far_out, far_in, near_send, near_recv, far_send, far_recv = scratch
    me, inner, outer, a, b, onward, _ = places_of(devices)
    partner = a * inner + (1 - b)
    meet([partner] + [place * inner + b for place in onward[:-1]], across)
    near, far = [], []
    for i, place in enumerate(onward):
        copy = pltpu.make_async_remote_copy(
            terms_ref.at[place * inner + (1 - b)], near_in.at[i],
            near_send.at[i], near_recv.at[i], **peer(partner),
        )
        copy.start()
        near.append(copy)
    if width:
        for copy in x_far + [x_own, keep]:
            copy.start()
    for i, place in enumerate(onward):
        near[i].wait_recv()
        both = terms_ref[place * inner + b].astype(jnp.float32) + near_in[i].astype(jnp.float32)
        if i == outer - 1:
            out_ref[...] = both
            break
        far_out[i] = both.astype(jnp.bfloat16)
        copy = pltpu.make_async_remote_copy(
            far_out.at[i], far_in.at[i], far_send.at[i], far_recv.at[i],
            **peer(place * inner + b),
        )
        copy.start()
        far.append(copy)
    if width:
        for i in range(len(x_far)):
            x_far[i].wait_recv()
            x_onto[i].start()
    for i, copy in enumerate(far):
        copy.wait_recv()
        out_ref[...] += far_in[i].astype(jnp.float32)
    for copy in near + far:
        copy.wait_send()
    if width:
        keep.wait()
        x_own.wait()
        for copy in x_far:
            copy.wait_send()
        for copy in x_onto:
            copy.wait()


def total(terms, ident, label, layer_input=None, whole=None):
    devices, rows, columns = terms.shape
    outer = devices // 2
    dma = pltpu.SemaphoreType.DMA
    vmem, anywhere = pl.BlockSpec(memory_space=pltpu.VMEM), pl.BlockSpec(memory_space=pl.ANY)
    out_shape = [jax.ShapeDtypeStruct((rows, columns), jnp.float32)]
    scratch = [
        pltpu.VMEM((outer, rows, columns), jnp.bfloat16),
        pltpu.VMEM((outer - 1, rows, columns), jnp.bfloat16),
        pltpu.VMEM((outer - 1, rows, columns), jnp.bfloat16),
        dma((outer,)), dma((outer,)), dma((outer - 1,)), dma((outer - 1,)),
    ]
    width, more, aliases = 0, [], {}
    if whole is not None:
        width = whole.shape[0]
        more, aliases = [layer_input, whole], {2: 1}
        out_shape.append(jax.ShapeDtypeStruct(whole.shape, whole.dtype))
        scratch += [dma] + gather_sems(width)
    return pl.pallas_call(
        functools.partial(total_kernel, devices, width),
        out_shape=out_shape,
        in_specs=[vmem] + [anywhere] * len(more),
        out_specs=[vmem] + [anywhere] * (len(out_shape) - 1),
        scratch_shapes=scratch,
        input_output_aliases=aliases,
        compiler_params=pltpu.CompilerParams(collective_id=ident, has_side_effects=True),
        name=label,
    )(terms, *more)


def gather_copies(devices, axis, mine, pool, own_send, own_recv, far_send, far_recv, pass_send, pass_recv):
    me, inner, outer, a, b, onward, source = places_of(devices, axis)
    partner = a * inner + (1 - b)
    own = pltpu.make_async_remote_copy(mine, pool(me), own_send, own_recv, **peer(partner, axis))
    far = [
        pltpu.make_async_remote_copy(
            mine, pool(me), far_send.at[i], far_recv.at[i], **peer(onward[i] * inner + b, axis)
        )
        for i in range(outer - 1)
    ]
    onto = [
        pltpu.make_async_remote_copy(
            pool(source[i] * inner + b), pool(source[i] * inner + b),
            pass_send.at[i], pass_recv.at[i], **peer(partner, axis),
        )
        for i in range(outer - 1)
    ]
    others = [partner] + [onward[i] * inner + b for i in range(outer - 1)]
    return own, far, onto, others


def gather_sems(devices):
    dma, hops = pltpu.SemaphoreType.DMA, devices // 2 - 1
    return [dma, dma, dma((hops,)), dma((hops,)), dma((hops,)), dma((hops,))]


def input_copies(width, start, count, x_ref, whole_ref, keep_sem, *sems):
    part = pl.ds(start, count)
    keep = pltpu.make_async_copy(x_ref.at[part], whole_ref.at[lax.axis_index("tp"), part], keep_sem)
    return keep, gather_copies(
        width, "tp", x_ref.at[part], lambda place: whole_ref.at[place, part], *sems
    )


def local_kernel(devices, width, steps, scale, mine_ref, x_ref, q_ref, k_ref, v_ref, o_ref, g_ref, log_ref, hide_ref,
                 dq_ref, dk_ref, dv_ref, delta_ref, pool_ref, whole_ref, *sems):
    positions = q_ref.shape[1]
    step = pl.program_id(0) * pl.num_programs(1) + pl.program_id(1)
    own, far, onto, others = gather_copies(
        devices, "kv", mine_ref, lambda place: pool_ref.at[place], *sems[:6]
    )
    keep, (x_own, x_far, x_onto, across) = input_copies(
        width, 0, x_ref.shape[0] // 2, x_ref, whole_ref, *sems[6:]
    )

    @pl.when(step == 0)
    def _():
        meet(others, across)
        for copy in far:
            copy.start()
        own.start()
        for copy in x_far + [x_own, keep]:
            copy.start()

    for i in range(len(far)):
        @pl.when(step == (i + 1) * steps // (len(far) + 1))
        def _(i=i):
            far[i].wait_recv()
            onto[i].start()

    product = g_ref[0].astype(jnp.float32) * o_ref[0].astype(jnp.float32)
    delta = jnp.sum(product.T, axis=0, keepdims=True)
    delta_ref[0, 0] = delta
    log_row = log_ref[0, 0]
    chunk = GROUP * BLK
    for start in range(0, positions, chunk):
        keys = slice(start, start + chunk)
        rest = slice(start, positions)
        shifts = [
            log_row[:, rest] + hide_ref[0, start // BLK + i : start // BLK + i + 1, rest]
            for i in range(GROUP)
        ]
        dq, dk, dv = pair_terms(
            k_ref[0, keys], v_ref[0, keys], q_ref[0, rest], g_ref[0, rest],
            shifts, delta[:, rest], scale, True,
        )
        if start == 0:
            dq_ref[0] = dq
        else:
            dq_ref[0, rest] += dq
        dk_ref[0, keys] = dk.astype(jnp.bfloat16)
        dv_ref[0, keys] = dv.astype(jnp.bfloat16)

    @pl.when(step == steps - 1)
    def _():
        own.wait()
        for copy in far:
            copy.wait_send()
        for copy in x_far:
            copy.wait_recv()
        for copy in x_onto:
            copy.start()
        for copy in onto:
            copy.wait()
        keep.wait()
        x_own.wait()
        for copy in x_far:
            copy.wait_send()
        for copy in x_onto:
            copy.wait()


def remote_kernel(scale, order_ref, read_ref, chunks_ref, pool_ref, hide_ref, q_ref, g_ref, log_ref,
                  delta_ref, base_ref, dq_ref, out_ref, total):
    s = pl.program_id(1)

    @pl.when(s == 0)
    def _():
        out_ref[...] = jnp.zeros_like(out_ref)

    total[...] = base_ref[0]

    @pl.loop(0, chunks_ref[s])
    def _(c):
        slots = [order_ref[s, c * GROUP + i] for i in range(GROUP)]
        places = [(lax.div(r, CAP), lax.rem(r, CAP)) for r in slots]
        reads = [read_ref[s, c * GROUP + i] for i in range(GROUP)]
        reads = [(lax.div(r, CAP), lax.rem(r, CAP)) for r in reads]
        k = jnp.concatenate([pool_ref[o, 0, n] for o, n in reads], axis=0)
        v = jnp.concatenate([pool_ref[o, 1, n] for o, n in reads], axis=0)
        shifts = [log_ref[0, 0] + hide_ref[r] for r in slots]
        dq, dk, dv = pair_terms(
            k, v, q_ref[0], g_ref[0], shifts, delta_ref[0, 0], scale, False
        )
        total[...] += dq
        dk = dk.astype(jnp.bfloat16)
        dv = dv.astype(jnp.bfloat16)
        for i, (o, n) in enumerate(places):
            out_ref[o, 0, n] = dk[i * BLK : (i + 1) * BLK]
            out_ref[o, 1, n] = dv[i * BLK : (i + 1) * BLK]

    dq_ref[0] = (total[...] * scale).astype(jnp.bfloat16)


def body(layer_input, queries, keys, values, outputs, d_out, log_sums, chosen):
    sequences, positions, channels = queries.shape
    head_count = log_sums.shape[2]
    head_size = channels // head_count
    local_blocks = positions // BLK
    devices = lax.axis_size("kv")
    me = lax.axis_index("kv")
    own_blocks = sequences * local_blocks
    slots = devices * CAP
    scale = head_size ** (-0.5)
    bf16, f32, i32 = jnp.bfloat16, jnp.float32, jnp.int32

    every = spread(chosen, devices).transpose(1, 0, 2, 3).reshape(sequences, -1, chosen.shape[2])
    width = lax.axis_size("tp")

    total_blocks = devices * local_blocks
    ids = jnp.arange(total_blocks, dtype=i32)
    asker = ids // local_blocks
    named = (every[..., None] == ids) & (
        asker[None, :, None, None] != asker[None, None, None, :]
    )
    needed = jnp.any(named, axis=(1, 2))
    needed = needed.reshape(sequences, devices, local_blocks).transpose(1, 0, 2)
    needed = needed.reshape(devices, own_blocks)
    place = jnp.where(needed, jnp.arange(own_blocks, dtype=i32), own_blocks)
    table = []
    for _ in range(CAP):
        first = jnp.min(place, axis=1)
        table.append(first)
        place = jnp.where(place == first[:, None], own_blocks, place)
    table = jnp.stack(table, axis=1)
    served = lax.dynamic_slice_in_dim(table, me, 1, 0).reshape(CAP)
    served = jnp.where(served < own_blocks, served, 0)

    key_rows = keys.reshape(own_blocks, BLK, channels)
    value_rows = values.reshape(own_blocks, BLK, channels)
    sent = jnp.stack([
        jnp.stack([lax.dynamic_index_in_dim(rows, served[n], 0, False) for n in range(CAP)])
        for rows in (key_rows, value_rows)
    ])

    slot_place = table.reshape(slots)
    slot_owner = jnp.arange(slots, dtype=i32) // CAP
    slot_ok = (slot_place < own_blocks) & (slot_owner != me)
    slot_seq = jnp.where(slot_ok, slot_place // local_blocks, -1)
    slot_block = slot_owner * local_blocks + slot_place % local_blocks
    seqs = jnp.arange(sequences, dtype=i32)
    sees = jnp.any(chosen[..., None] == slot_block, axis=2) & (
        slot_seq[None, None, :] == seqs[:, None, None]
    )
    seen = jnp.any(sees, axis=0)
    remote_hide = jnp.where(seen.T, 0.0, HIDDEN).astype(f32)
    remote_hide = jnp.repeat(remote_hide, BLK, axis=1).reshape(slots, 1, positions)
    match = jnp.any(sees, axis=1)
    line = jnp.arange(slots, dtype=i32)
    rank = jnp.sum((match[:, None, :] & (line[None, None, :] < line[None, :, None])).astype(i32), axis=2)
    count = jnp.sum(match.astype(i32), axis=1)
    chunks = (count + GROUP - 1) // GROUP
    padded = -(-slots // GROUP) * GROUP
    steps = jnp.arange(padded, dtype=i32)
    hits = match[:, None, :] & (rank[:, None, :] == steps[None, :, None])
    order = jnp.sum(jnp.where(hits, line[None, None, :], 0), axis=2)
    filled = steps[None, :] < count[:, None]
    read = jnp.where(filled, order, (me ^ 1) * CAP)
    order = jnp.where(filled, order, me * CAP)

    mine = me * local_blocks + jnp.arange(local_blocks, dtype=i32)
    near = jnp.any(chosen[..., None] == mine, axis=2)
    local_hide = jnp.where(near.transpose(0, 2, 1), 0.0, HIDDEN).astype(f32)
    local_hide = jnp.repeat(local_hide, BLK, axis=2)
    log_rows = (log_sums * LOG2E).transpose(0, 2, 1)[:, :, None, :]

    tile = pl.BlockSpec((1, positions, head_size), lambda s, h: (s, 0, h))
    row = pl.BlockSpec((1, 1, 1, positions), lambda s, h: (s, h, 0, 0))
    shape = (sequences, positions, channels)
    flops = 10 * sequences * head_count * positions * positions * head_size
    anywhere = pl.BlockSpec(memory_space=pl.ANY)
    dq_local, dk_local, dv_local, delta_rows, pool, whole_input = pl.pallas_call(
        functools.partial(local_kernel, devices, width, sequences * head_count, scale),
        grid=(sequences, head_count),
        in_specs=[anywhere] * 2 + [tile] * 5 + [row, pl.BlockSpec((1, local_blocks, positions), lambda s, h: (s, 0, 0))],
        out_specs=[tile, tile, tile, row, anywhere, anywhere],
        out_shape=[
            jax.ShapeDtypeStruct(shape, f32),
            jax.ShapeDtypeStruct(shape, bf16),
            jax.ShapeDtypeStruct(shape, bf16),
            jax.ShapeDtypeStruct((sequences, head_count, 1, positions), f32),
            jax.ShapeDtypeStruct((devices, 2, CAP, BLK, channels), bf16),
            jax.ShapeDtypeStruct((width,) + layer_input.shape, bf16),
        ],
        scratch_shapes=gather_sems(devices) + [pltpu.SemaphoreType.DMA] + gather_sems(width),
        compiler_params=pltpu.CompilerParams(collective_id=1, has_side_effects=True),
        cost_estimate=pl.CostEstimate(flops=4 * flops, bytes_accessed=queries.size * 18, transcendentals=0),
        name="near_terms",
    )(sent, layer_input, queries, keys, values, outputs, d_out, log_rows, local_hide)

    tile_t = pl.BlockSpec((1, positions, head_size), lambda h, s, *_: (s, 0, h))
    row_t = pl.BlockSpec((1, 1, 1, positions), lambda h, s, *_: (s, h, 0, 0))
    pool_t = pl.BlockSpec((devices, 2, CAP, BLK, head_size), lambda h, s, *_: (0, 0, 0, 0, h))
    d_queries, terms = pl.pallas_call(
        functools.partial(remote_kernel, scale),
        grid_spec=pltpu.PrefetchScalarGridSpec(
            num_scalar_prefetch=3,
            grid=(head_count, sequences),
            in_specs=[
                pool_t,
                pl.BlockSpec((slots, 1, positions), lambda h, s, *_: (0, 0, 0)),
                tile_t, tile_t, row_t, row_t, tile_t,
            ],
            out_specs=[tile_t, pool_t],
            scratch_shapes=[pltpu.VMEM((positions, head_size), f32)],
        ),
        out_shape=[
            jax.ShapeDtypeStruct(shape, bf16),
            jax.ShapeDtypeStruct((devices, 2, CAP, BLK, channels), bf16),
        ],
        cost_estimate=pl.CostEstimate(flops=2 * flops, bytes_accessed=queries.size * 10, transcendentals=0),
        name="far_terms",
    )(order, read, chunks, pool, remote_hide, queries, d_out, log_rows, delta_rows, dq_local)

    returned, whole_input = total(
        terms.reshape(devices, 2 * CAP * BLK, channels), 2, "return_terms", layer_input, whole_input
    )
    returned = returned.reshape(2, CAP, BLK, channels)

    def settle(rows, back):
        rows = rows.reshape(own_blocks, BLK, channels).astype(f32)
        block = jnp.arange(own_blocks, dtype=i32)[:, None, None]
        for n in range(CAP):
            rows = rows + jnp.where(block == served[n], back[n][None], 0.0)
        return rows.astype(bf16).reshape(shape)

    d_keys = settle(dk_local, returned[0])
    d_values = settle(dv_local, returned[1])
    input_rows = whole_input.reshape(-1, sequences * positions, layer_input.shape[2])
    partial = jnp.einsum(
        "pti,tj->pij", input_rows, d_values.reshape(sequences * positions, channels),
        preferred_element_type=f32,
    ).astype(bf16).reshape(devices, -1, channels)
    d_weight, = total(partial, 3, "weight_terms")
    return (d_queries, d_keys, d_values, d_weight)


def solution(mesh):
    split = P(None, "kv", "tp")
    return jax.shard_map(
        body,
        mesh=mesh,
        in_specs=(split,) * 7 + (P(None, "kv", None),),
        out_specs=(split, split, split, P("kv", "tp")),
        check_vma=False,
    )
```
